32 devices in a mesh: sp: 8 (over z, y), tp: 4 (over x, core).
Axes of the slice: x: 2, y: 2, z: 4, core: 2. Of those that a mesh axis runs over, the one named last changes fastest.
Arguments:
- queries: bfloat16 [4096, 1024], P('sp', 'tp'), may hold values from -6 to 6
- keys: bfloat16 [4096, 1024], P('sp', 'tp'), may hold values from -6 to 6
- values: bfloat16 [4096, 1024], P('sp', 'tp'), may hold values from -6 to 6
- cum_gate: float32 [4096, 16], P('sp', 'tp'), as said below
- documents: int32 [4096], P('sp'), may hold values from 0 to 3, never falling along the last dimension, each value on 1 to 2048 neighbouring positions
- head_gain: float32 [1024], P('tp'), may hold values from 0.1 to 1.9
- out_weight: bfloat16 [1024, 2048], replicated, may hold values from -0.1875 to 0.1875
- resid: bfloat16 [4096, 2048], P(('sp', 'tp')), may hold values from -6 to 6
- norm_gain: float32 [2048], replicated, may hold values from 0.1 to 1.9
- routes: int32 [4096, 2], P(('sp', 'tp')), may hold values from 0 to 7, all different within a row; in each aligned block of 128 rows (0 to 127, 128 to 255, ...) at most 64 rows name the same one
- route_weights: float32 [4096, 2], P(('sp', 'tp')), may hold values from 0.25 to 1
- w_gate: bfloat16 [8, 2048, 3584], P('sp', None, 'tp'), may hold values from -0.125 to 0.125
- w_up: bfloat16 [8, 2048, 3584], P('sp', None, 'tp'), may hold values from -0.125 to 0.125
- w_down: bfloat16 [8, 3584, 2048], P('sp', 'tp'), may hold values from -0.09375 to 0.09375
Outputs:
- mixed: bfloat16 [4096, 2048], P(('sp', 'tp'))
The draws below stay inside these ranges and needn't reach their ends.
Inputs may be any that keep to these rules, and one draw needn't show every extreme that they name: `cum_gate`: along the positions each head's values never rise. `documents`: document numbers never fall along the positions. `routes`: the 2 experts of a row differ. In each aligned block of 128 rows no expert is named more than 64 times; in some blocks an expert is named exactly 64 times.
All inputs are finite; a program needn't handle non-finite values.
Results may differ from the reference program's by a relative error of at most 0.015.
Values may be sent and summed in bfloat16 or wider, within the bound.
A program may use at most 128 MiB of HBM per device.

```python
import math
import jax
import jax.numpy as jnp
import numpy as np
from jax import lax

D = 2048
HEADS = 16
HEAD_DIM = 64
FFE = 3584
TOP = 2
TOK_DEV = 512
SEQUENCE_LENGTH = 4096
ROWS_DEV = 128
HD = 1024
EXPERTS = 8
CAP = 64
SLICE = 896
N_SP = 8
N_TP = 4


def draw_queries(key, part):
    drawn = jax.random.normal(jax.random.fold_in(key, 1), (SEQUENCE_LENGTH, HEADS * HEAD_DIM), jnp.float32)
    return jnp.clip(drawn, -6.0, 6.0).astype(jnp.bfloat16)


def draw_keys(key, part):
    drawn = jax.random.normal(jax.random.fold_in(key, 2), (SEQUENCE_LENGTH, HEADS * HEAD_DIM), jnp.float32)
    return jnp.clip(drawn, -6.0, 6.0).astype(jnp.bfloat16)


def draw_cum_gate(key, part):
    head_order = jax.random.permutation(jax.random.fold_in(key, 21), HEADS)
    fast_heads = head_order < HEADS // 2
    quick_decay_rate = jnp.exp(jax.random.uniform(jax.random.fold_in(key, 22), (HEADS,), jnp.float32, math.log(0.03), math.log(0.08)))
    slow_rate = jax.random.uniform(jax.random.fold_in(key, 23), (HEADS,), jnp.float32, 0.3, 0.8) / SEQUENCE_LENGTH
    head_rates = jnp.where(fast_heads, quick_decay_rate, slow_rate)
    blocks = SEQUENCE_LENGTH // TOK_DEV
    factor = jnp.exp(jax.random.uniform(jax.random.fold_in(key, 24), (blocks, HEADS), jnp.float32, -0.7, 0.7))
    factor = jnp.repeat(factor, TOK_DEV, axis=0)
    jitter = jax.random.uniform(jax.random.fold_in(key, 25), (SEQUENCE_LENGTH, HEADS), jnp.float32, 0.5, 1.5)
    logged_step_list = -head_rates[None, :] * factor * jitter
    spike_position = jax.random.randint(jax.random.fold_in(key, 26), (3,), 0, SEQUENCE_LENGTH)
    loss_values = jax.random.uniform(jax.random.fold_in(key, 27), (3, HEADS), jnp.float32, 0.2, 0.5)
    logged_step_list = logged_step_list.at[spike_position].add(jnp.log(1.0 - loss_values))
    return jnp.cumsum(logged_step_list, axis=0)


def block_scale(stream_key, shape, shards, smallest, high):
    factor_of = 1.0
    for axis_at, shards_of in shards:
        heights = jax.random.uniform(jax.random.fold_in(jax.random.fold_in(stream_key, 6), axis_at), (shards_of,), jnp.float32, smallest / len(shards), high / len(shards))
        factor_of = factor_of * jnp.repeat(jnp.exp(heights), shape[axis_at] // shards_of).reshape((-1,) + (1,) * (len(shape) - 1 - axis_at))
    return factor_of


def length_profile(count, total, reach, slope):
    loads = [(1 << 20) // math.isqrt(rank ** slope) + 1 for rank in range(2, count + 1)]
    spare, given = total - reach - (count - 1), [1] * (count - 1)
    while spare > 0:
        candidates = [i for i in range(count - 1) if given[i] < reach]
        pool, left = sum([loads[i] for i in candidates]), spare
        for i in candidates:
            addition = min(reach - given[i], max(1, left * loads[i] // pool), spare)
            given[i] = given[i] + addition
            spare = spare - addition
    return np.array([reach] + given)


def ragged_sizes(own_key, count, total, bound, lean):
    if count == 2:
        one = jax.random.randint(own_key, (), max(1, total - bound), min(bound, total - 1) + 1)
        return jnp.stack([one, total - one])
    sizes = jnp.asarray(length_profile(count, total, bound, lean), jnp.int32)
    twos = (count - 1) // 2
    source_of, taker = sizes[1:1 + 2 * twos:2], sizes[2:2 + 2 * twos:2]
    margin = jnp.minimum(source_of - 1, bound - taker)
    shifted = jax.random.randint(jax.random.fold_in(own_key, 1), (twos,), 0, 1 << 20) % (margin + 1)
    sizes = sizes.at[1:1 + 2 * twos:2].set(source_of - shifted).at[2:2 + 2 * twos:2].set(taker + shifted)
    return sizes[jax.random.permutation(jax.random.fold_in(own_key, 2), count)]


def shared_out(own_key, own, number, rows, count, top, most, lean):
    sequence = jax.random.permutation(own_key, count)
    heavy_load, usual = shares(count, rows * top, most, lean, True), shares(count, rows * top, most, lean, False)
    places = jnp.arange(count)

    def named(tallies, offset_by):
        used = int((tallies > 0).sum())
        fixed = max(1, used // 4)
        passed = fixed + (places - fixed + offset_by * (used - fixed)) % max(1, count - fixed)
        return jnp.zeros((count,), jnp.int32).at[sequence[jnp.where(places < fixed, places, passed)]].set(jnp.asarray(tallies, jnp.int32))

    tallies = jnp.where(number % 4 == 0, named(heavy_load, number // 4), named(usual, number - number // 4 - 1))
    mixed = jax.random.permutation(jax.random.fold_in(own, 3), count)
    source_of, sink = mixed[0:count // 2 * 2:2], mixed[1:count // 2 * 2:2]
    room = jnp.minimum(tallies[source_of] - 1, most - tallies[sink]) // 2
    room = jnp.where((source_of == sequence[0]) | (sink == sequence[0]) | (tallies[sink] == 0), 0, jnp.maximum(room, 0))
    passed = jax.random.randint(jax.random.fold_in(own, 4), (count // 2,), 0, 1 << 20) % (room + 1)
    tallies = tallies.at[source_of].add(-passed).at[sink].add(passed)
    labels = jnp.searchsorted(jnp.cumsum(tallies), jnp.arange(rows * top), side="right").astype(jnp.int32)
    table = labels.reshape(top, rows).T
    table = table[jax.random.permutation(jax.random.fold_in(own, 1), rows)]
    offset_by = jax.random.randint(jax.random.fold_in(own, 2), (rows, 1), 0, top)
    return jnp.take_along_axis(table, (jnp.arange(top)[None, :] + offset_by) % top, axis=1)


def shares(amount, total, limit, slope, full):
    portions = [(1 << 20) // math.isqrt(grade ** slope) + 1 for grade in range(1, amount + 1)]
    largest = limit if full else min(limit, max(-(-total // amount), total * portions[0] // sum(portions)))
    least = 1 if total - largest >= amount - 1 else 0
    counts, spare = [largest] + [least] * (amount - 1), total - largest - least * (amount - 1)
    while spare > 0:
        free = [i for i in range(1, amount) if counts[i] < largest] or [i for i in range(1, amount) if counts[i] < limit]
        whole, remaining = sum([portions[i] for i in free]), spare
        for i in free:
            extra = min(limit - counts[i], max(1, remaining * portions[i] // whole), spare)
            counts[i] = counts[i] + extra
            spare = spare - extra
    return np.array(counts)


def noise(stream_key, dims, spread, bound, split=(), held_as=jnp.bfloat16):
    entries = jax.random.normal(stream_key, dims, jnp.float32) * spread
    if len(split) > 0:
        entries = block_scale(stream_key, dims, split, -0.22, 0.18) * entries
    return jnp.clip(entries, min=-bound, max=bound).astype(held_as)


def setup_inputs(seed: int = 0) -> dict:
    seeds = jax.random.split(jax.random.key(seed), 15)
    queries = draw_queries(jax.random.fold_in(seeds[14], 71), 0)
    keys = draw_keys(jax.random.fold_in(seeds[14], 71), 0)
    values = noise(seeds[2], (SEQUENCE_LENGTH, HD), 1.0, 6.0, ((0, 8), (1, 4)))
    cum_gate = draw_cum_gate(jax.random.fold_in(seeds[14], 71), 0)
    documents = jnp.searchsorted(jnp.cumsum(ragged_sizes(seeds[4], 4, SEQUENCE_LENGTH, SEQUENCE_LENGTH // 2, 2)), jnp.arange(SEQUENCE_LENGTH), side="right").astype(jnp.int32)
    head_gain = jnp.clip(1.0 + 0.18 * jax.random.normal(seeds[5], (HD,), jnp.float32), 0.1, 1.9)
    out_weight = noise(seeds[6], (HD, D), HD ** -0.5, 0.1875)
    resid = noise(seeds[7], (SEQUENCE_LENGTH, D), 1.0, 6.0, ((0, 32),))
    norm_gain = jnp.clip(1.0 + 0.18 * jax.random.normal(seeds[8], (D,), jnp.float32), 0.1, 1.9)
    routes_keys = jax.random.split(jax.random.fold_in(seeds[9], 1), SEQUENCE_LENGTH // ROWS_DEV)
    routes_turns = jax.random.permutation(jax.random.fold_in(seeds[9], 3), SEQUENCE_LENGTH // ROWS_DEV)
    routes = jax.vmap(lambda own, number: shared_out(jax.random.fold_in(seeds[9], 2), own, number, ROWS_DEV, EXPERTS, TOP, CAP, 2))(routes_keys, routes_turns).reshape((SEQUENCE_LENGTH, TOP))
    route_weights = jnp.clip(jnp.exp(math.log(1.0) - 1.3862944 * jax.random.uniform(seeds[10], (SEQUENCE_LENGTH, TOP), jnp.float32) ** block_scale(seeds[10], (SEQUENCE_LENGTH, TOP), ((0, 32),), -0.2, 0.2)), 0.25, 1.0)
    w_gate = noise(seeds[11], (EXPERTS, D, FFE), D ** -0.5, 0.125, ((0, 8), (2, 4)))
    w_up = noise(seeds[12], (EXPERTS, D, FFE), D ** -0.5, 0.125, ((0, 8), (2, 4)))
    w_down = noise(seeds[13], (EXPERTS, FFE, D), FFE ** -0.5, 0.09375, ((0, 8), (1, 4)))
    return dict(queries=queries, keys=keys, values=values, cum_gate=cum_gate, documents=documents, head_gain=head_gain, out_weight=out_weight, resid=resid, norm_gain=norm_gain, routes=routes, route_weights=route_weights, w_gate=w_gate, w_up=w_up, w_down=w_down)


EPS = 1e-06

def attention(queries, keys, values, cum_gate, documents):
    block_len = math.gcd(SEQUENCE_LENGTH, 256)
    block_count = SEQUENCE_LENGTH // block_len
    key_heads = keys.reshape(SEQUENCE_LENGTH, HEADS, HEAD_DIM).astype(jnp.float32)
    value_heads = values.reshape(SEQUENCE_LENGTH, HEADS, HEAD_DIM).astype(jnp.float32)
    positions = jnp.arange(SEQUENCE_LENGTH, dtype=jnp.int32)
    score_scale = HEAD_DIM ** (-0.5)

    def one_block(block_index):
        first_pos = block_index * block_len
        query_row_block = lax.dynamic_slice_in_dim(queries, first_pos, block_len, 0)
        query_row_block = query_row_block.reshape(block_len, HEADS, HEAD_DIM).astype(jnp.float32)
        gate_here = lax.dynamic_slice_in_dim(cum_gate, first_pos, block_len, 0)
        doc_here = lax.dynamic_slice_in_dim(documents, first_pos, block_len, 0)
        query_pos = first_pos + jnp.arange(block_len, dtype=jnp.int32)
        scores = jnp.einsum('qhd,khd->qhk', query_row_block, key_heads) * score_scale
        scores = scores + gate_here[:, :, None] - cum_gate.T[None, :, :]
        allowed = (positions[None, :] <= query_pos[:, None]) & (documents[None, :] == doc_here[:, None])
        scores = jnp.where(allowed[:, None, :], scores, -jnp.inf)
        row_max = lax.optimization_barrier(jnp.max(scores, axis=-1, keepdims=True))
        exp_scores = jnp.exp(scores - row_max)
        row_sum = lax.optimization_barrier(jnp.sum(exp_scores, axis=-1))
        weights = lax.optimization_barrier(exp_scores.astype(jnp.bfloat16)).astype(jnp.float32)
        return jnp.einsum('qhk,khd->qhd', weights, value_heads) / row_sum[:, :, None]
    attended = lax.map(one_block, jnp.arange(block_count, dtype=jnp.int32))
    return attended.reshape(SEQUENCE_LENGTH, HEADS, HEAD_DIM)

def experts_out(expert_input, routes, w_gate, w_up, w_down):
    capacity = N_SP * N_TP * CAP
    flat_routes = routes.reshape(-1)
    route_total = flat_routes.shape[0]
    owners = jnp.arange(route_total, dtype=jnp.int32) // TOP

    def one_expert(expert_index):
        matches = (flat_routes == expert_index).astype(jnp.int32)
        ranks = jnp.cumsum(matches) - 1
        slots = jnp.where(matches == 1, ranks, capacity)
        slot_owner = jnp.zeros((capacity + 1,), jnp.int32).at[slots].set(owners)[:capacity]
        picked = expert_input[slot_owner]
        gate_out = jnp.dot(picked, w_gate[expert_index], preferred_element_type=jnp.float32)
        up_out = jnp.dot(picked, w_up[expert_index], preferred_element_type=jnp.float32)
        hidden = (jax.nn.silu(gate_out) * up_out).astype(jnp.bfloat16)
        pieces = hidden.reshape(capacity, N_TP, SLICE).astype(jnp.float32)
        down_blocks = w_down[expert_index].reshape(N_TP, SLICE, D).astype(jnp.float32)
        partial_value = jnp.einsum('rjf,jfd->jrd', pieces, down_blocks)
        partial_value = lax.optimization_barrier(partial_value.astype(jnp.bfloat16)).astype(jnp.float32)
        return lax.optimization_barrier(jnp.sum(partial_value, axis=0)).astype(jnp.bfloat16)
    results = lax.map(one_expert, jnp.arange(EXPERTS, dtype=jnp.int32))
    onehot = (flat_routes[:, None] == jnp.arange(EXPERTS, dtype=jnp.int32)[None, :]).astype(jnp.int32)
    ranks = lax.optimization_barrier(jnp.sum(jnp.cumsum(onehot, axis=0) * onehot, axis=1)) - 1
    return results[flat_routes, ranks].reshape(SEQUENCE_LENGTH, TOP, D)

def reference(queries, keys, values, cum_gate, documents, head_gain, out_weight, resid, norm_gain, routes, route_weights, w_gate, w_up, w_down):
    attended = attention(queries, keys, values, cum_gate, documents)
    mean_square = lax.optimization_barrier(jnp.mean(attended * attended, axis=-1, keepdims=True))
    head_normed = (attended * lax.rsqrt(mean_square + EPS)).reshape(SEQUENCE_LENGTH, HEADS * HEAD_DIM) * head_gain
    head_normed = head_normed.astype(jnp.bfloat16)
    projected = jnp.dot(head_normed, out_weight, preferred_element_type=jnp.float32)
    stream = lax.optimization_barrier((resid.astype(jnp.float32) + projected).astype(jnp.bfloat16))
    widened = stream.astype(jnp.float32)
    mean_wide = lax.optimization_barrier(jnp.mean(widened * widened, axis=-1, keepdims=True))
    expert_input = (widened * lax.rsqrt(mean_wide + EPS) * norm_gain).astype(jnp.bfloat16)
    gathered = experts_out(expert_input, routes, w_gate, w_up, w_down)
    mixed = widened + lax.optimization_barrier(jnp.sum(route_weights[:, :, None] * gathered.astype(jnp.float32), axis=1))
    return mixed.astype(jnp.bfloat16)
```

```python
import functools

import jax
import jax.numpy as jnp
from jax import lax
from jax.experimental import pallas as pl
from jax.experimental.pallas import tpu as pltpu
from jax.sharding import PartitionSpec as P

EPS = 1e-06
MESH = pl.DeviceIdType.MESH
NEG = -1e30
VMEM_LIMIT = 60 * 1024 * 1024


def attention_kernel(
    heads_here, block_len, first_ref, q_ref, kv_ref, gate_ref, start_ref, gain_ref, out_ref
):
    tokens, width_here = q_ref.shape
    head_size = width_here // heads_here
    score_scale = head_size ** (-0.5)
    first_block, own_block = first_ref[0], first_ref[1]
    blocks_own = tokens // block_len

    def visit(head, rows, offset, state, causal):
        cols = slice(head * head_size, (head + 1) * head_size)
        vcols = slice(width_here + head * head_size, width_here + (head + 1) * head_size)
        row_max, row_sum, weighted = state
        offset = pl.multiple_of(offset, block_len)
        k = kv_ref[pl.ds(offset, block_len), cols]
        v = kv_ref[pl.ds(offset, block_len), vcols]
        gate = gate_ref[head : head + 1, pl.ds(offset, block_len)]
        base = gate_ref[head : head + 1, pl.ds(pl.multiple_of(own_block * tokens, tokens), 128)][
            :, :1
        ]
        scores = (
            lax.dot_general(
                q_ref[rows, cols],
                k,
                (((1,), (1,)), ((), ())),
                preferred_element_type=jnp.float32,
            )
            * score_scale
        )
        scores = scores + (base - gate)
        key_pos = offset + lax.broadcasted_iota(jnp.int32, (1, block_len), 1)
        allowed = key_pos >= start_ref[rows, :]
        if causal:
            query_pos = (
                own_block * tokens
                + rows.start
                + lax.broadcasted_iota(jnp.int32, (block_len, 1), 0)
            )
            allowed = allowed & (key_pos <= query_pos)
        scores = jnp.where(allowed, scores, NEG)
        next_max = jnp.maximum(row_max, jnp.max(scores, axis=-1, keepdims=True))
        exps = jnp.exp(scores - next_max)
        rescale = jnp.exp(row_max - next_max)
        row_sum = row_sum * rescale + jnp.sum(exps, axis=-1, keepdims=True)
        weighted = weighted * rescale + jnp.dot(
            exps.astype(jnp.bfloat16), v, preferred_element_type=jnp.float32
        )
        return next_max, row_sum, weighted

    for part in range(blocks_own):
        rows = slice(part * block_len, (part + 1) * block_len)
        outs = []
        for head in range(heads_here):
            state = (
                jnp.full((block_len, 1), NEG, jnp.float32),
                jnp.zeros((block_len, 1), jnp.float32),
                jnp.zeros((block_len, head_size), jnp.float32),
            )
            diagonal = own_block * blocks_own + part
            state = visit(head, rows, diagonal * block_len, state, True)
            state = lax.fori_loop(
                first_block,
                diagonal,
                lambda j, s: visit(head, rows, j * block_len, s, False),
                state,
            )
            attended = state[2] / state[1]
            mean_square = jnp.mean(attended * attended, axis=-1, keepdims=True)
            outs.append(attended * lax.rsqrt(mean_square + EPS))
        normed = jnp.concatenate(outs, axis=-1) * gain_ref[...]
        out_ref[rows, :] = normed.astype(jnp.bfloat16)


def expert_kernel(
    n,
    out_ref,
    wg_hbm,
    wu_hbm,
    wd_hbm,
    ret_ref,
    fan,
    wg,
    wu,
    wd,
    hidden,
    part,
    got,
    pair,
    across,
    fin,
    w_sem,
    own_sem,
    a_send,
    a_recv,
    x_send,
    x_recv,
    c_send,
    c_recv,
    d_send,
    d_recv,
    p_send,
    p_recv,
    s_send,
    s_recv,
    r_send,
    r_recv,
):
    me = lax.axis_index("sp")
    t = lax.axis_index("tp")
    c, xi = lax.rem(t, 2), t // 2
    near = xi * 2 + (1 - c)
    far = (1 - xi) * 2 + c
    cap, width = out_ref.shape[1], out_ref.shape[2]
    near_id = {"sp": me, "tp": near}
    far_id = {"sp": me, "tp": far}

    weights = [
        pltpu.make_async_copy(src, dst, w_sem.at[i])
        for i, (src, dst) in enumerate(((wg_hbm, wg), (wu_hbm, wu), (wd_hbm, wd)))
    ]
    for copy in weights:
        copy.start()

    barrier = pltpu.get_barrier_semaphore()

    def greet(k, carry):
        pl.semaphore_signal(
            barrier,
            inc=1,
            device_id={"sp": lax.rem(me + k, n), "tp": t},
            device_id_type=MESH,
        )
        return carry

    lax.fori_loop(1, n, greet, 0)
    for other in (near_id, far_id):
        pl.semaphore_signal(barrier, inc=1, device_id=other, device_id_type=MESH)
    pl.semaphore_wait(barrier, n + 1)

    def remote(src, dst, send, recv, to):
        return pltpu.make_async_remote_copy(
            src_ref=src, dst_ref=dst, send_sem=send, recv_sem=recv, device_id=to, device_id_type=MESH
        )

    def source(k):
        return lax.rem(me - k + n, n)

    def a_out(k):
        to = lax.rem(me + k, n)
        return remote(
            out_ref.at[to], fan.at[me, t], a_send.at[k], a_recv.at[me], {"sp": to, "tp": t}
        )

    def a_in(k):
        p = source(k)
        return remote(out_ref.at[p], fan.at[p, t], a_send.at[k], a_recv.at[p], near_id)

    def x_copy(k, q):
        p = source(k)
        return remote(fan.at[p, q], fan.at[p, q], x_send.at[p], x_recv.at[p], far_id)

    def c_copy(k, q):
        p = source(k)
        return remote(fan.at[p, q], fan.at[p, q], c_send.at[p], c_recv.at[p], near_id)

    def d_copy(k, q):
        p = source(k)
        return remote(fan.at[p, q], fan.at[p, q], d_send.at[p], d_recv.at[p], near_id)

    def p_copy(k):
        p = source(k)
        return remote(part.at[p, 1 - c], got.at[p], p_send.at[p], p_recv.at[p], near_id)

    def s_copy(k):
        p = source(k)
        return remote(pair.at[p], across.at[p], s_send.at[p], s_recv.at[p], far_id)

    def r_out(k):
        p = source(k)
        return remote(fin.at[p], ret_ref.at[me], r_send.at[p], r_recv.at[me], {"sp": p, "tp": t})

    def r_in(k):
        p = source(k)
        return remote(fin.at[p], ret_ref.at[p], r_send.at[p], r_recv.at[p], near_id)

    own = pltpu.make_async_copy(out_ref.at[me], fan.at[me, t], own_sem)
    own.start()
    lax.fori_loop(1, n, lambda k, z: (a_out(k).start(), z)[1], 0)

    def forward(k):
        x_copy(k, t).start()
        c_copy(k, t).start()

    own.wait()
    forward(0)

    def step_a(k):
        a_in(k).wait_recv()
        forward(k)

    def step_x(k):
        x_copy(k, far).wait_recv()
        d_copy(k, far).start()

    def step_compute(k):
        p = source(k)
        c_copy(k, near).wait_recv()
        d_copy(k, 3 - t).wait_recv()
        rows = fan[p].reshape(4 * cap, width)
        gate = jnp.dot(rows, wg[...], preferred_element_type=jnp.float32)
        up = jnp.dot(rows, wu[...], preferred_element_type=jnp.float32)
        hidden[...] = (gate * jax.nn.sigmoid(gate) * up).astype(jnp.bfloat16)
        tile = 512 if width % 512 == 0 else width
        for at in range(0, width, tile):
            down = jnp.dot(
                hidden[...], wd[:, at : at + tile], preferred_element_type=jnp.float32
            ).astype(jnp.bfloat16)
            for q in range(4):
                part[p, q % 2, q // 2, :, at : at + tile] = down[q * cap : (q + 1) * cap]
        p_copy(k).start()

    def step_pair(k):
        p = source(k)
        p_copy(k).wait_recv()
        pair[p] = (
            part[p, c, 1 - xi].astype(jnp.float32) + got[p, 1 - xi].astype(jnp.float32)
        ).astype(jnp.bfloat16)
        s_copy(k).start()

    def step_final(k):
        p = source(k)
        s_copy(k).wait_recv()
        total = (
            part[p, c, xi].astype(jnp.float32)
            + got[p, xi].astype(jnp.float32)
            + across[p].astype(jnp.float32)
        ).astype(jnp.bfloat16)

        @pl.when(k == 0)
        def _():
            ret_ref[me] = total

        @pl.when(k > 0)
        def _():
            fin[p] = total
            r_out(k).start()

    step_a(1)
    step_x(0)
    for copy in weights:
        copy.wait()

    def iteration(i, carry):
        @pl.when(i + 2 < n)
        def _():
            step_a(i + 2)

        @pl.when(i + 1 < n)
        def _():
            step_x(i + 1)

        @pl.when((i >= 1) & (i < n + 1))
        def _():
            step_pair(i - 1)

        @pl.when(i < n)
        def _():
            step_compute(i)

        @pl.when(i >= 2)
        def _():
            step_final(i - 2)

        return carry

    lax.fori_loop(0, n + 2, iteration, 0)

    def finish(k, carry):
        x_copy(k, t).wait_send()
        c_copy(k, t).wait_send()
        d_copy(k, far).wait_send()
        p_copy(k).wait_send()
        s_copy(k).wait_send()

        @pl.when(k > 0)
        def _():
            a_out(k).wait_send()
            r_out(k).wait_send()
            r_in(k).wait_recv()

        return carry

    lax.fori_loop(0, n, finish, 0)


def experts(n, outbound, w_gate, w_up, w_down):
    _, cap, width = outbound.shape
    hid = w_gate.shape[1]
    bf = jnp.bfloat16
    dma = pltpu.SemaphoreType.DMA
    hbm = pl.BlockSpec(memory_space=pl.ANY)
    vmem = pl.BlockSpec(memory_space=pltpu.VMEM)
    return pl.pallas_call(
        functools.partial(expert_kernel, n),
        out_shape=jax.ShapeDtypeStruct((n, cap, width), bf),
        in_specs=[vmem, hbm, hbm, hbm],
        out_specs=vmem,
        scratch_shapes=[
            pltpu.VMEM((n, 4, cap, width), bf),
            pltpu.VMEM((width, hid), bf),
            pltpu.VMEM((width, hid), bf),
            pltpu.VMEM((hid, width), bf),
            pltpu.VMEM((4 * cap, hid), bf),
            pltpu.VMEM((n, 2, 2, cap, width), bf),
            pltpu.VMEM((n, 2, cap, width), bf),
            pltpu.VMEM((n, cap, width), bf),
            pltpu.VMEM((n, cap, width), bf),
            pltpu.VMEM((n, cap, width), bf),
            dma((3,)),
            dma,
        ]
        + [dma((n,)) for _ in range(14)],
        compiler_params=pltpu.CompilerParams(
            collective_id=1, has_side_effects=True, vmem_limit_bytes=VMEM_LIMIT
        ),
    )(outbound, w_gate, w_up, w_down)


def on_device(
    queries,
    keys,
    values,
    cum_gate,
    documents,
    head_gain,
    out_weight,
    resid,
    norm_gain,
    routes,
    route_weights,
    w_gate,
    w_up,
    w_down,
):
    bf = jnp.bfloat16
    tokens = queries.shape[0]
    heads_here = cum_gate.shape[1]
    width_here = queries.shape[1]
    me = lax.axis_index("sp")
    high = lax.reduce_precision(cum_gate, 8, 7)
    middle = lax.reduce_precision(cum_gate - high, 8, 7)
    low = cum_gate - high - middle
    extra = jnp.concatenate(
        [high, middle, low, documents[:, None].astype(jnp.float32)], axis=1
    ).astype(bf)
    pad = -extra.shape[1] % 128
    packed = jnp.concatenate([keys, values, jnp.pad(extra, ((0, 0), (0, pad)))], axis=1)
    packed = lax.all_gather(packed, "sp", axis=0, tiled=True)
    tail = packed[:, 2 * width_here :].astype(jnp.float32)
    gates = (
        tail[:, :heads_here]
        + tail[:, heads_here : 2 * heads_here]
        + tail[:, 2 * heads_here : 3 * heads_here]
    ).T
    all_docs = tail[:, 3 * heads_here].astype(jnp.int32)
    starts = jnp.sum(
        (all_docs[None, :] < documents[:, None]).astype(jnp.int32), axis=1, keepdims=True
    )
    block_len = min(tokens, 512)
    first = jnp.stack([starts[0, 0] // block_len, me]).astype(jnp.int32)
    vmem = pl.BlockSpec(memory_space=pltpu.VMEM)
    head_normed = pl.pallas_call(
        functools.partial(attention_kernel, heads_here, block_len),
        out_shape=jax.ShapeDtypeStruct((tokens, width_here), bf),
        in_specs=[pl.BlockSpec(memory_space=pltpu.SMEM)] + [vmem] * 5,
        out_specs=vmem,
        compiler_params=pltpu.CompilerParams(vmem_limit_bytes=VMEM_LIMIT),
    )(first, queries, packed, gates, starts, head_gain[None, :])

    regrouped = lax.all_to_all(head_normed, "tp", split_axis=0, concat_axis=1, tiled=True)
    projected = jnp.dot(regrouped, out_weight, preferred_element_type=jnp.float32)
    stream = lax.optimization_barrier((resid.astype(jnp.float32) + projected).astype(bf))
    widened = stream.astype(jnp.float32)
    mean_wide = jnp.mean(widened * widened, axis=-1, keepdims=True)
    expert_input = (widened * lax.rsqrt(mean_wide + EPS) * norm_gain).astype(bf)

    local_rows, top_count = routes.shape
    expert_count = lax.axis_size("sp")
    tp_count = lax.axis_size("tp")
    capacity = 2 * top_count * tokens // (tp_count * expert_count)
    flat_routes = routes.reshape(-1)
    onehot = (flat_routes[:, None] == jnp.arange(expert_count, dtype=jnp.int32)[None, :]).astype(
        jnp.float32
    )
    order = jnp.arange(flat_routes.shape[0], dtype=jnp.int32)
    earlier = (order[None, :] < order[:, None]).astype(bf)
    counts = jnp.dot(earlier, onehot.astype(bf), preferred_element_type=jnp.float32)
    ranks = jnp.sum(counts * onehot, axis=1).astype(jnp.int32)
    targets = (flat_routes * capacity + ranks).reshape(local_rows, top_count)
    slots = jnp.arange(expert_count * capacity, dtype=jnp.int32)
    picks = targets[:, :, None] == slots[None, None, :]
    into = jnp.any(picks, axis=1).astype(bf)
    outbound = lax.dot_general(
        into, expert_input, (((0,), (0,)), ((), ())), preferred_element_type=jnp.float32
    ).astype(bf)
    outbound = outbound.reshape(expert_count, capacity, -1)
    returned = experts(expert_count, outbound, w_gate[0], w_up[0], w_down[0])
    returned = returned.reshape(expert_count * capacity, -1)
    mixed = widened
    for route in range(top_count):
        chosen = jnp.dot(
            picks[:, route].astype(bf), returned, preferred_element_type=jnp.float32
        )
        mixed = mixed + route_weights[:, route : route + 1] * chosen
    return mixed.astype(bf)


def solution(mesh):
    in_specs = (
        P("sp", "tp"),
        P("sp", "tp"),
        P("sp", "tp"),
        P("sp", "tp"),
        P("sp"),
        P("tp"),
        P(),
        P(("sp", "tp"), None),
        P(),
        P(("sp", "tp"), None),
        P(("sp", "tp"), None),
        P("sp", None, "tp"),
        P("sp", None, "tp"),
        P("sp", "tp", None),
    )
    out_specs = P(("sp", "tp"), None)
    return jax.shard_map(
        on_device, mesh=mesh, in_specs=in_specs, out_specs=out_specs, check_vma=False
    )
```

```python
import functools

import jax
import jax.numpy as jnp
from jax import lax
from jax.experimental import pallas as pl
from jax.experimental.pallas import tpu as pltpu
from jax.sharding import PartitionSpec as P

EPS = 1e-06
MESH = pl.DeviceIdType.MESH
NEG = -1e30
VMEM_LIMIT = 60 * 1024 * 1024


def attention_kernel(
    heads_here, block_len, first_ref, q_ref, kv_ref, gate_ref, start_ref, gain_ref, out_ref
):
    tokens, width_here = q_ref.shape
    head_size = width_here // heads_here
    score_scale = head_size ** (-0.5)
    first_block, own_block = first_ref[0], first_ref[1]
    blocks_own = tokens // block_len

    def visit(head, rows, offset, state, causal):
        cols = slice(head * head_size, (head + 1) * head_size)
        vcols = slice(width_here + head * head_size, width_here + (head + 1) * head_size)
        row_max, row_sum, weighted = state
        offset = pl.multiple_of(offset, block_len)
        k = kv_ref[pl.ds(offset, block_len), cols]
        v = kv_ref[pl.ds(offset, block_len), vcols]
        gate = gate_ref[head : head + 1, pl.ds(offset, block_len)]
        base = gate_ref[head : head + 1, pl.ds(pl.multiple_of(own_block * tokens, tokens), 128)][
            :, :1
        ]
        scores = (
            lax.dot_general(
                q_ref[rows, cols],
                k,
                (((1,), (1,)), ((), ())),
                preferred_element_type=jnp.float32,
            )
            * score_scale
        )
        scores = scores + (base - gate)
        key_pos = offset + lax.broadcasted_iota(jnp.int32, (1, block_len), 1)
        allowed = key_pos >= start_ref[rows, :]
        if causal:
            query_pos = (
                own_block * tokens
                + rows.start
                + lax.broadcasted_iota(jnp.int32, (block_len, 1), 0)
            )
            allowed = allowed & (key_pos <= query_pos)
        scores = jnp.where(allowed, scores, NEG)
        next_max = jnp.maximum(row_max, jnp.max(scores, axis=-1, keepdims=True))
        exps = jnp.exp(scores - next_max)
        rescale = jnp.exp(row_max - next_max)
        row_sum = row_sum * rescale + jnp.sum(exps, axis=-1, keepdims=True)
        weighted = weighted * rescale + jnp.dot(
            exps.astype(jnp.bfloat16), v, preferred_element_type=jnp.float32
        )
        return next_max, row_sum, weighted

    for part in range(blocks_own):
        rows = slice(part * block_len, (part + 1) * block_len)
        outs = []
        for head in range(heads_here):
            state = (
                jnp.full((block_len, 1), NEG, jnp.float32),
                jnp.zeros((block_len, 1), jnp.float32),
                jnp.zeros((block_len, head_size), jnp.float32),
            )
            diagonal = own_block * blocks_own + part
            state = visit(head, rows, diagonal * block_len, state, True)
            state = lax.fori_loop(
                first_block,
                diagonal,
                lambda j, s: visit(head, rows, j * block_len, s, False),
                state,
            )
            attended = state[2] / state[1]
            mean_square = jnp.mean(attended * attended, axis=-1, keepdims=True)
            outs.append(attended * lax.rsqrt(mean_square + EPS))
        normed = jnp.concatenate(outs, axis=-1) * gain_ref[...]
        out_ref[rows, :] = normed.astype(jnp.bfloat16)


def expert_kernel(
    n,
    out_ref,
    wg_hbm,
    wu_hbm,
    wd_hbm,
    ret_ref,
    fan,
    wg,
    wu,
    wd,
    hidden,
    part,
    got,
    pair,
    across,
    fin,
    w_sem,
    own_sem,
    a_send,
    a_recv,
    x_send,
    x_recv,
    c_send,
    c_recv,
    d_send,
    d_recv,
    p_send,
    p_recv,
    s_send,
    s_recv,
    r_send,
    r_recv,
):
    me = lax.axis_index("sp")
    t = lax.axis_index("tp")
    c, xi = lax.rem(t, 2), t // 2
    near = xi * 2 + (1 - c)
    far = (1 - xi) * 2 + c
    cap, width = out_ref.shape[1], out_ref.shape[2]
    near_id = {"sp": me, "tp": near}
    far_id = {"sp": me, "tp": far}

    weights = [
        pltpu.make_async_copy(src, dst, w_sem.at[i])
        for i, (src, dst) in enumerate(((wg_hbm, wg), (wu_hbm, wu), (wd_hbm, wd)))
    ]
    for copy in weights:
        copy.start()

    barrier = pltpu.get_barrier_semaphore()

    def greet(k, carry):
        pl.semaphore_signal(
            barrier,
            inc=1,
            device_id={"sp": lax.rem(me + k, n), "tp": t},
            device_id_type=MESH,
        )
        return carry

    lax.fori_loop(1, n, greet, 0)
    for other in (near_id, far_id):
        pl.semaphore_signal(barrier, inc=1, device_id=other, device_id_type=MESH)
    pl.semaphore_wait(barrier, n + 1)

    def remote(src, dst, send, recv, to):
        return pltpu.make_async_remote_copy(
            src_ref=src, dst_ref=dst, send_sem=send, recv_sem=recv, device_id=to, device_id_type=MESH
        )

    def source(k):
        return lax.rem(me - k + n, n)

    def a_out(k):
        to = lax.rem(me + k, n)
        return remote(
            out_ref.at[to], fan.at[me, t], a_send.at[k], a_recv.at[me], {"sp": to, "tp": t}
        )

    def a_in(k):
        p = source(k)
        return remote(out_ref.at[p], fan.at[p, t], a_send.at[k], a_recv.at[p], near_id)

    def x_copy(k, q):
        p = source(k)
        return remote(fan.at[p, q], fan.at[p, q], x_send.at[p], x_recv.at[p], far_id)

    def c_copy(k, q):
        p = source(k)
        return remote(fan.at[p, q], fan.at[p, q], c_send.at[p], c_recv.at[p], near_id)

    def d_copy(k, q):
        p = source(k)
        return remote(fan.at[p, q], fan.at[p, q], d_send.at[p], d_recv.at[p], near_id)

    def p_copy(k):
        p = source(k)
        return remote(part.at[p, 1 - c], got.at[p], p_send.at[p], p_recv.at[p], near_id)

    def s_copy(k):
        p = source(k)
        return remote(pair.at[p], across.at[p], s_send.at[p], s_recv.at[p], far_id)

    def r_out(k):
        p = source(k)
        return remote(fin.at[p], ret_ref.at[me], r_send.at[p], r_recv.at[me], {"sp": p, "tp": t})

    def r_in(k):
        p = source(k)
        return remote(fin.at[p], ret_ref.at[p], r_send.at[p], r_recv.at[p], near_id)

    own = pltpu.make_async_copy(out_ref.at[me], fan.at[me, t], own_sem)
    own.start()
    lax.fori_loop(1, n, lambda k, z: (a_out(k).start(), z)[1], 0)

    def forward(k):
        x_copy(k, t).start()
        c_copy(k, t).start()

    own.wait()
    forward(0)

    def step_a(k):
        a_in(k).wait_recv()
        forward(k)

    def step_x(k):
        x_copy(k, far).wait_recv()
        d_copy(k, far).start()

    def step_compute(k):
        p = source(k)
        c_copy(k, near).wait_recv()
        d_copy(k, 3 - t).wait_recv()
        rows = fan[p].reshape(4 * cap, width)
        gate = jnp.dot(rows, wg[...], preferred_element_type=jnp.float32)
        up = jnp.dot(rows, wu[...], preferred_element_type=jnp.float32)
        hidden[...] = (gate * jax.nn.sigmoid(gate) * up).astype(jnp.bfloat16)
        tile = 512 if width % 512 == 0 else width
        for at in range(0, width, tile):
            down = jnp.dot(
                hidden[...], wd[:, at : at + tile], preferred_element_type=jnp.float32
            ).astype(jnp.bfloat16)
            for q in range(4):
                part[p, q % 2, q // 2, :, at : at + tile] = down[q * cap : (q + 1) * cap]
        p_copy(k).start()

    def step_pair(k):
        p = source(k)
        p_copy(k).wait_recv()
        pair[p] = (
            part[p, c, 1 - xi].astype(jnp.float32) + got[p, 1 - xi].astype(jnp.float32)
        ).astype(jnp.bfloat16)
        s_copy(k).start()

    def step_final(k):
        p = source(k)
        s_copy(k).wait_recv()
        total = (
            part[p, c, xi].astype(jnp.float32)
            + got[p, xi].astype(jnp.float32)
            + across[p].astype(jnp.float32)
        ).astype(jnp.bfloat16)

        @pl.when(k == 0)
        def _():
            ret_ref[me] = total

        @pl.when(k > 0)
        def _():
            fin[p] = total
            r_out(k).start()

    step_a(1)
    step_x(0)
    for copy in weights:
        copy.wait()

    def iteration(i, carry):
        @pl.when(i + 2 < n)
        def _():
            step_a(i + 2)

        @pl.when(i + 1 < n)
        def _():
            step_x(i + 1)

        @pl.when((i >= 1) & (i < n + 1))
        def _():
            step_pair(i - 1)

        @pl.when(i < n)
        def _():
            step_compute(i)

        @pl.when(i >= 2)
        def _():
            step_final(i - 2)

        return carry

    lax.fori_loop(0, n + 2, iteration, 0)

    def finish(k, carry):
        x_copy(k, t).wait_send()
        c_copy(k, t).wait_send()
        d_copy(k, far).wait_send()
        p_copy(k).wait_send()
        s_copy(k).wait_send()

        @pl.when(k > 0)
        def _():
            a_out(k).wait_send()
            r_out(k).wait_send()
            r_in(k).wait_recv()

        return carry

    lax.fori_loop(0, n, finish, 0)


def experts(n, outbound, w_gate, w_up, w_down):
    _, cap, width = outbound.shape
    hid = w_gate.shape[1]
    bf = jnp.bfloat16
    dma = pltpu.SemaphoreType.DMA
    hbm = pl.BlockSpec(memory_space=pl.ANY)
    vmem = pl.BlockSpec(memory_space=pltpu.VMEM)
    return pl.pallas_call(
        functools.partial(expert_kernel, n),
        out_shape=jax.ShapeDtypeStruct((n, cap, width), bf),
        in_specs=[vmem, hbm, hbm, hbm],
        out_specs=vmem,
        scratch_shapes=[
            pltpu.VMEM((n, 4, cap, width), bf),
            pltpu.VMEM((width, hid), bf),
            pltpu.VMEM((width, hid), bf),
            pltpu.VMEM((hid, width), bf),
            pltpu.VMEM((4 * cap, hid), bf),
            pltpu.VMEM((n, 2, 2, cap, width), bf),
            pltpu.VMEM((n, 2, cap, width), bf),
            pltpu.VMEM((n, cap, width), bf),
            pltpu.VMEM((n, cap, width), bf),
            pltpu.VMEM((n, cap, width), bf),
            dma((3,)),
            dma,
        ]
        + [dma((n,)) for _ in range(14)],
        compiler_params=pltpu.CompilerParams(
            collective_id=1, has_side_effects=True, vmem_limit_bytes=VMEM_LIMIT
        ),
    )(outbound, w_gate, w_up, w_down)


def history_kernel(n, own_ref, all_ref, own_sem, up_send, up_recv, mate_send, mate_recv):
    me = lax.axis_index("sp")
    y, z = lax.rem(me, 2), me // 2
    floors, reach = n // 2, n // 4
    mate_id = {"sp": me + 1 - 2 * y}
    above_id = {"sp": lax.rem(me + 2, n)}
    below_id = {"sp": lax.rem(me + n - 2, n)}
    barrier = pltpu.get_barrier_semaphore()
    for other in (mate_id, above_id, below_id):
        pl.semaphore_signal(barrier, inc=1, device_id=other, device_id_type=MESH)
    pl.semaphore_wait(barrier, 3)

    def remote(src, block, send, recv, to):
        return pltpu.make_async_remote_copy(
            src_ref=src,
            dst_ref=all_ref.at[block],
            send_sem=send,
            recv_sem=recv,
            device_id=to,
            device_id_type=MESH,
        )

    def up(d, src, block):
        return remote(src, block, up_send.at[d], up_recv.at[d], above_id)

    def over(d, src, block):
        return remote(src, block, mate_send.at[d], mate_recv.at[d], mate_id)

    own = pltpu.make_async_copy(own_ref, all_ref.at[me], own_sem)
    own.start()

    def sends(d):
        rising = (z + 1 < floors) & (z >= d) if d < reach else None
        if d == 0:
            crossing = y == 0
        elif d == reach:
            crossing = (y == 1) & (z >= d)
        else:
            crossing = z >= d
        return rising, crossing

    def block_of(d):
        return jnp.maximum(me - 2 * d, 0)

    for d in range(reach + 1):
        src = own_ref if d == 0 else all_ref.at[block_of(d)]
        if d > 0:
            @pl.when(z >= d)
            def _():
                up(d - 1, src, block_of(d)).wait_recv()

        rising, crossing = sends(d)
        if rising is not None:
            @pl.when(rising)
            def _():
                up(d, src, block_of(d)).start()

        @pl.when(crossing)
        def _():
            over(d, src, block_of(d)).start()

    for d in range(reach + 1):
        src = own_ref if d == 0 else all_ref.at[block_of(d)]
        theirs = jnp.maximum(me + 1 - 2 * y - 2 * d, 0)
        if d == 0:
            coming = y == 1
        elif d == reach:
            coming = (y == 0) & (z >= d)
        else:
            coming = z >= d

        @pl.when(coming)
        def _():
            over(d, own_ref, theirs).wait_recv()

        rising, crossing = sends(d)
        if rising is not None:
            @pl.when(rising)
            def _():
                up(d, src, block_of(d)).wait_send()

        @pl.when(crossing)
        def _():
            over(d, src, block_of(d)).wait_send()

    own.wait()


def gather_history(n, packed):
    tokens, wide = packed.shape
    steps = n // 4 + 1
    dma = pltpu.SemaphoreType.DMA
    gathered = pl.pallas_call(
        functools.partial(history_kernel, n),
        out_shape=jax.ShapeDtypeStruct((n, tokens, wide), packed.dtype),
        in_specs=[pl.BlockSpec(memory_space=pltpu.VMEM)],
        out_specs=pl.BlockSpec(memory_space=pl.ANY),
        scratch_shapes=[dma] + [dma((steps,)) for _ in range(4)],
        compiler_params=pltpu.CompilerParams(collective_id=2, has_side_effects=True),
    )(packed)
    return gathered.reshape(n * tokens, wide)


def on_device(
    queries,
    keys,
    values,
    cum_gate,
    documents,
    head_gain,
    out_weight,
    resid,
    norm_gain,
    routes,
    route_weights,
    w_gate,
    w_up,
    w_down,
):
    bf = jnp.bfloat16
    tokens = queries.shape[0]
    heads_here = cum_gate.shape[1]
    width_here = queries.shape[1]
    me = lax.axis_index("sp")
    high = lax.reduce_precision(cum_gate, 8, 7)
    middle = lax.reduce_precision(cum_gate - high, 8, 7)
    low = cum_gate - high - middle
    extra = jnp.concatenate(
        [high, middle, low, documents[:, None].astype(jnp.float32)], axis=1
    ).astype(bf)
    pad = -extra.shape[1] % 128
    packed = jnp.concatenate([keys, values, jnp.pad(extra, ((0, 0), (0, pad)))], axis=1)
    n = lax.axis_size("sp")
    packed = gather_history(n, packed)
    tail = packed[:, 2 * width_here :].astype(jnp.float32)
    gates = (
        tail[:, :heads_here]
        + tail[:, heads_here : 2 * heads_here]
        + tail[:, 2 * heads_here : 3 * heads_here]
    ).T
    all_docs = tail[:, 3 * heads_here].astype(jnp.int32)
    oldest = jnp.maximum(me - n // 2, 0) * tokens
    position = jnp.arange(n * tokens, dtype=jnp.int32)
    held = (position >= oldest) & (position < (me + 1) * tokens)
    before = (all_docs[None, :] < documents[:, None]) & held[None, :]
    starts = oldest + jnp.sum(before.astype(jnp.int32), axis=1, keepdims=True)
    block_len = min(tokens, 512)
    first = jnp.stack([starts[0, 0] // block_len, me]).astype(jnp.int32)
    vmem = pl.BlockSpec(memory_space=pltpu.VMEM)
    head_normed = pl.pallas_call(
        functools.partial(attention_kernel, heads_here, block_len),
        out_shape=jax.ShapeDtypeStruct((tokens, width_here), bf),
        in_specs=[pl.BlockSpec(memory_space=pltpu.SMEM)] + [vmem] * 5,
        out_specs=vmem,
        compiler_params=pltpu.CompilerParams(vmem_limit_bytes=VMEM_LIMIT),
    )(first, queries, packed, gates, starts, head_gain[None, :])

    regrouped = lax.all_to_all(head_normed, "tp", split_axis=0, concat_axis=1, tiled=True)
    projected = jnp.dot(regrouped, out_weight, preferred_element_type=jnp.float32)
    stream = lax.optimization_barrier((resid.astype(jnp.float32) + projected).astype(bf))
    widened = stream.astype(jnp.float32)
    mean_wide = jnp.mean(widened * widened, axis=-1, keepdims=True)
    expert_input = (widened * lax.rsqrt(mean_wide + EPS) * norm_gain).astype(bf)

    local_rows, top_count = routes.shape
    expert_count = lax.axis_size("sp")
    tp_count = lax.axis_size("tp")
    capacity = 2 * top_count * tokens // (tp_count * expert_count)
    flat_routes = routes.reshape(-1)
    onehot = (flat_routes[:, None] == jnp.arange(expert_count, dtype=jnp.int32)[None, :]).astype(
        jnp.float32
    )
    order = jnp.arange(flat_routes.shape[0], dtype=jnp.int32)
    earlier = (order[None, :] < order[:, None]).astype(bf)
    counts = jnp.dot(earlier, onehot.astype(bf), preferred_element_type=jnp.float32)
    ranks = jnp.sum(counts * onehot, axis=1).astype(jnp.int32)
    targets = (flat_routes * capacity + ranks).reshape(local_rows, top_count)
    slots = jnp.arange(expert_count * capacity, dtype=jnp.int32)
    picks = targets[:, :, None] == slots[None, None, :]
    into = jnp.any(picks, axis=1).astype(bf)
    outbound = lax.dot_general(
        into, expert_input, (((0,), (0,)), ((), ())), preferred_element_type=jnp.float32
    ).astype(bf)
    outbound = outbound.reshape(expert_count, capacity, -1)
    returned = experts(expert_count, outbound, w_gate[0], w_up[0], w_down[0])
    returned = returned.reshape(expert_count * capacity, -1)
    mixed = widened
    for route in range(top_count):
        chosen = jnp.dot(
            picks[:, route].astype(bf), returned, preferred_element_type=jnp.float32
        )
        mixed = mixed + route_weights[:, route : route + 1] * chosen
    return mixed.astype(bf)


def solution(mesh):
    in_specs = (
        P("sp", "tp"),
        P("sp", "tp"),
        P("sp", "tp"),
        P("sp", "tp"),
        P("sp"),
        P("tp"),
        P(),
        P(("sp", "tp"), None),
        P(),
        P(("sp", "tp"), None),
        P(("sp", "tp"), None),
        P("sp", None, "tp"),
        P("sp", None, "tp"),
        P("sp", "tp", None),
    )
    out_specs = P(("sp", "tp"), None)
    return jax.shard_map(
        on_device, mesh=mesh, in_specs=in_specs, out_specs=out_specs, check_vma=False
    )
```
